32 devices in a mesh: fs: 8 (over z, x), tp: 4 (over y, core).
Axes of the slice: x: 2, y: 2, z: 4, core: 2. Of those that a mesh axis runs over, the one named last changes fastest.
Arguments:
- x_late: bfloat16 [3072, 2048], P(('fs', 'tp')), may hold values from -6 to 6
- x_early: bfloat16 [3072, 2048], P(('fs', 'tp')), may hold values from -6 to 6
- cotangent: bfloat16 [3072, 2048], P(('fs', 'tp')), may hold values from -6 to 6
- up_weight: bfloat16 [2048, 4096], P('fs', 'tp'), may hold values from -0.125 to 0.125
- down_weight: bfloat16 [2048, 4096], P('fs', 'tp'), may hold values from -0.09375 to 0.09375
- up_grad_sum: float32 [2048, 4096], P('fs', 'tp'), may hold values from -24 to 24
- down_grad_sum: float32 [2048, 4096], P('fs', 'tp'), may hold values from -24 to 24
Outputs:
- output: bfloat16 [3072, 2048], P(('fs', 'tp'))
- input_grad: bfloat16 [3072, 2048], P(('fs', 'tp'))
- up_grad_new: float32 [2048, 4096], P('fs', 'tp')
- down_grad_new: float32 [2048, 4096], P('fs', 'tp')
The draws below stay inside these ranges and needn't reach their ends.
All inputs are finite; a program needn't handle non-finite values.
Results may differ from the reference program's by a relative error of at most 0.0095.
Values may be sent and summed in bfloat16 or wider, within the bound.
A program may use at most 128 MiB of HBM per device.

```python
import jax
import jax.numpy as jnp
from jax import lax

D = 2048
FF = 4096
TOKENS = 3072
N_TP = 4


def raised(result, rng, source, target, shards_of, factor):
    owner, partner = [(jnp.arange(result.shape[axis_at]) // (result.shape[axis_at] // shards_of)).reshape([-1 if axis == axis_at else 1 for axis in range(result.ndim)]) for axis_at in (source, target)]
    chosen = jax.random.permutation(rng, shards_of)[partner]
    strong = (owner == chosen) | (owner == (partner + shards_of // 2) % shards_of)
    return jnp.where(strong, factor * result, result)


def block_levels(stream_key, extent, split, low, top_value):
    def one(position, shards_of):
        draws = jax.random.uniform(jax.random.fold_in(jax.random.fold_in(stream_key, 6), position), (shards_of,), jnp.float32, low / len(split), top_value / len(split))
        return jnp.repeat(jnp.exp(draws), extent[position] // shards_of).reshape((-1,) + (1,) * (len(extent) - position - 1))

    level = one(*split[0])
    for cut in split[1:]:
        level = level * one(*cut)
    return level


def normal_values(stream_key, dims, scale, limit, cuts=(), dtype=jnp.bfloat16):
    entries = jax.random.normal(stream_key, dims, jnp.float32) * scale
    if len(cuts) > 0:
        entries = block_levels(stream_key, dims, cuts, -0.22, 0.18) * entries
    return jnp.clip(entries, min=-limit, max=limit).astype(dtype)


def noise_with(own_key, extent, deviation, reach, pieces, heavy, dtype=jnp.bfloat16):
    drawn = deviation * jax.random.normal(own_key, extent, jnp.float32)
    if pieces:
        drawn = drawn * block_levels(own_key, extent, pieces, -0.22, 0.18)
    return jnp.clip(raised(drawn, jax.random.fold_in(own_key, 3), *heavy), -reach, reach).astype(dtype)


def setup_inputs(seed: int = 0) -> dict:
    arg_keys = jax.random.split(jax.random.key(seed), 8)
    x_late = normal_values(arg_keys[0], (TOKENS, D), 1.0, 6.0, ((0, 32),))
    x_early = normal_values(arg_keys[1], (TOKENS, D), 1.0, 6.0, ((0, 32),))
    cotangent = noise_with(arg_keys[2], (TOKENS, D), 0.25, 6.0, ((0, 32),), (0, 1, 32, 2.75))
    up_weight = normal_values(arg_keys[3], (D, FF), D ** -0.5, 0.125, ((0, 8), (1, 4)))
    down_weight = normal_values(arg_keys[4], (D, FF), FF ** -0.5, 0.09375, ((0, 8), (1, 4)))
    up_grad_sum = normal_values(arg_keys[5], (D, FF), 4.0, 24.0, ((0, 8), (1, 4)), jnp.float32)
    down_grad_sum = normal_values(arg_keys[6], (D, FF), 4.0, 24.0, ((0, 8), (1, 4)), jnp.float32)
    return dict(x_late=x_late, x_early=x_early, cotangent=cotangent, up_weight=up_weight, down_weight=down_weight, up_grad_sum=up_grad_sum, down_grad_sum=down_grad_sum)


def dot_last(left, right):
    return lax.dot_general(left, right, (((1,), (1,)), ((), ())), preferred_element_type=jnp.float32)


def dot_first(left, right):
    return lax.dot_general(left, right, (((0,), (0,)), ((), ())), preferred_element_type=jnp.float32)


def tp_rounded(left, right):
    stride = right.shape[1] // N_TP
    totals = jnp.zeros((left.shape[0], right.shape[0]), jnp.float32)
    for column_block in range(N_TP):
        first_col = column_block * stride
        partial_value = dot_last(left[:, first_col:first_col + stride], right[:, first_col:first_col + stride])
        rounded = lax.optimization_barrier(partial_value.astype(jnp.bfloat16))
        totals = totals + rounded.astype(jnp.float32)
    return totals.astype(jnp.bfloat16)


def reference(x_late, x_early, cotangent, up_weight, down_weight, up_grad_sum, down_grad_sum):
    pre_late = jnp.dot(x_late, up_weight, preferred_element_type=jnp.float32)
    act_late = jnp.square(jax.nn.relu(pre_late)).astype(jnp.bfloat16)
    output = tp_rounded(act_late, down_weight)
    pre_early = jnp.dot(x_early, up_weight, preferred_element_type=jnp.float32)
    act_early = jnp.square(jax.nn.relu(pre_early)).astype(jnp.bfloat16)
    grad_act = jnp.dot(cotangent, down_weight, preferred_element_type=jnp.float32)
    grad_pre = (grad_act * 2.0 * jax.nn.relu(pre_early)).astype(jnp.bfloat16)
    input_grad = tp_rounded(grad_pre, up_weight)
    up_grad_new = up_grad_sum + dot_first(x_early, grad_pre)
    down_grad_new = down_grad_sum + dot_first(cotangent, act_early)
    return (output, input_grad, up_grad_new, down_grad_new)
```

```python
import functools

import jax
import jax.numpy as jnp
from jax import lax
from jax.experimental import pallas as pl
from jax.experimental.pallas import tpu as pltpu
from jax.sharding import PartitionSpec as P


MESH = pl.DeviceIdType.MESH
ANY = pl.BlockSpec(memory_space=pl.ANY)
VMEM = pl.BlockSpec(memory_space=pltpu.VMEM)


def dot_last(left, right):
    return lax.dot_general(
        left, right, (((1,), (1,)), ((), ())), preferred_element_type=jnp.float32
    )


def dot_first(left, right):
    return lax.dot_general(
        left, right, (((0,), (0,)), ((), ())), preferred_element_type=jnp.float32
    )


def squared(pre_act):
    return jnp.square(jax.nn.relu(pre_act)).astype(jnp.bfloat16)


def hidden_grad(grad_act, pre_early):
    return (grad_act * 2.0 * jax.nn.relu(pre_early)).astype(jnp.bfloat16)


def flip(value, bit):
    return value + bit - 2 * bit * ((value // bit) % 2)


def remote(src, dst, send, recv, fs, tp):
    return pltpu.make_async_remote_copy(
        src_ref=src, dst_ref=dst, send_sem=send, recv_sem=recv,
        device_id={"fs": fs, "tp": tp}, device_id_type=MESH,
    )


def greet(peers):
    barrier = pltpu.get_barrier_semaphore()
    for fs, tp in peers:
        pl.semaphore_signal(barrier, inc=1, device_id={"fs": fs, "tp": tp}, device_id_type=MESH)
    pl.semaphore_wait(barrier, len(peers))


def gather_kernel(n_fo, n_tp, *refs):
    tokens, weights = refs[0:3], refs[3:5]
    all_tokens, all_weights = refs[5:8], refs[8:10]
    local, t_send, t_recv, x_send, x_recv, z_send, z_recv = refs[10:]
    fs, tp = lax.axis_index("fs"), lax.axis_index("tp")
    fo, fi = fs // 2, fs % 2
    pair = fo * 2 + 1 - fi
    half = weights[0].shape[1] // 2
    dims = n_tp.bit_length()

    def placed(mask):
        at_fi, at_tp = (1 - fi if mask & 1 else fi), tp
        for dim in range(1, dims):
            if (mask >> dim) & 1:
                at_tp = flip(at_tp, n_tp >> dim)
        return at_fi, at_tp

    def token(a, dim, mask):
        to_fi, to_tp = placed(1 << dim)
        slot = placed(mask)
        dst = all_tokens[a].at[slot[0], slot[1]]
        sem = mask + (1 << dim)
        return remote(tokens[a] if mask == 0 else dst, dst, t_send.at[a, sem], t_recv.at[a, sem],
                      fo * 2 + to_fi, to_tp)

    def columns(w, which):
        return weights[w].at[:, pl.ds(pl.multiple_of(which * half, half), half)]

    def across(w):
        return remote(columns(w, 1 - fi), all_weights[w].at[fs], x_send.at[w], x_recv.at[w], pair, tp)

    def along(w, step, part):
        dst = all_weights[w].at[pair if part else fs]
        return remote(dst if part else columns(w, fi), dst, z_send.at[w, step - 1, part],
                      z_recv.at[w, step - 1, part], ((fo + step) % n_fo) * 2 + fi, tp)

    peers = []
    for dim in range(dims):
        to_fi, to_tp = placed(1 << dim)
        peers.append((fo * 2 + to_fi, to_tp))
    for step in range(1, n_fo):
        peers.append((((fo + step) % n_fo) * 2 + fi, tp))
    greet(peers)

    for a in range(3):
        token(a, 0, 0).start()
        if a < 2:
            across(a).start()
    for w in range(2):
        for step in range(1, n_fo):
            along(w, step, 0).start()
    for a in range(3):
        for dim in range(1, dims):
            token(a, dim, 0).start()
    own = [pltpu.make_async_copy(tokens[a], all_tokens[a].at[fi, tp], local.at[a]) for a in range(3)]
    own += [pltpu.make_async_copy(columns(w, fi), all_weights[w].at[fs], local.at[3 + w]) for w in range(2)]
    for copy in own:
        copy.start()

    for dim in range(dims):
        for a in range(3):
            for mask in range(1 << dim):
                token(a, dim, mask).wait_recv()
                for later in range(dim + 1, dims):
                    token(a, later, mask + (1 << dim)).start()
            if dim == 0 and a < 2:
                across(a).wait_recv()
                for step in range(1, n_fo):
                    along(a, step, 1).start()
    for w in range(2):
        across(w).wait_send()
        for step in range(1, n_fo):
            for part in range(2):
                along(w, step, part).wait()
    for dim in range(dims):
        for a in range(3):
            for mask in range(1 << dim):
                token(a, dim, mask).wait_send()
    for copy in own:
        copy.wait()


def gather(n_fo, n_tp, tokens, weights):
    rows, width = tokens[0].shape
    w_rows, cols = weights[0].shape
    masks = 2 * n_tp
    dma = pltpu.SemaphoreType.DMA
    return pl.pallas_call(
        functools.partial(gather_kernel, n_fo, n_tp),
        out_shape=[jax.ShapeDtypeStruct((2, n_tp, rows, width), jnp.bfloat16)] * 3
        + [jax.ShapeDtypeStruct((2 * n_fo, w_rows, cols // 2), jnp.bfloat16)] * 2,
        in_specs=[VMEM] * 5,
        out_specs=[ANY] * 5,
        scratch_shapes=[
            dma((5,)), dma((3, masks)), dma((3, masks)), dma((2,)), dma((2,)),
            dma((2, n_fo - 1, 2)), dma((2, n_fo - 1, 2)),
        ],
        compiler_params=pltpu.CompilerParams(collective_id=0, has_side_effects=True),
        name="gather",
    )(*tokens, *weights)


def reduce_kernel(n_fo, n_tp, *refs):
    partial, grads = refs[0:2], refs[2:4]
    summed, mine, other = refs[4:6], refs[6:8], refs[8:10]
    (landed, pair_sum, arrived, g_in, staged,
     c_send, c_recv, t_send, t_recv, z_send, z_recv, x_send, x_recv) = refs[10:]
    fs, tp = lax.axis_index("fs"), lax.axis_index("tp")
    fo, fi = fs // 2, fs % 2
    pair = fo * 2 + 1 - fi
    n_y = n_tp // 2
    y, core = tp // 2, tp % 2
    others = [(dx, dy) for dy in range(n_y) for dx in range(2) if (dx, dy) != (0, 0)]

    def spot(dx, dy):
        return (1 - fi if dx else fi), (y + dy) % n_y

    def near(a):
        return remote(partial[a].at[:, :, 1 - core], landed.at[a], c_send.at[a], c_recv.at[a],
                      fs, y * 2 + 1 - core)

    def far(a, k):
        at_fi, at_y = spot(*others[k])
        return remote(pair_sum.at[a, at_fi, at_y], arrived.at[a, k], t_send.at[a, k], t_recv.at[a, k],
                      fo * 2 + at_fi, at_y * 2 + core)

    def along(w, step):
        to_fo = (fo + step) % n_fo
        return remote(grads[w].at[to_fo], g_in.at[w, step - 1], z_send.at[w, step - 1],
                      z_recv.at[w, step - 1], to_fo * 2 + fi, tp)

    def across(w):
        return remote(staged.at[w], other[w], x_send.at[w], x_recv.at[w], pair, tp)

    peers = [(fs, y * 2 + 1 - core)]
    for dx, dy in others:
        at_fi, at_y = spot(dx, dy)
        peers.append((fo * 2 + at_fi, at_y * 2 + core))
    for step in range(1, n_fo):
        peers.append((((fo + step) % n_fo) * 2 + fi, tp))
    greet(peers)

    for a in range(2):
        near(a).start()
    for w in range(2):
        for step in range(1, n_fo):
            along(w, step).start()

    def joined(a, at_fi, at_y):
        return (partial[a][at_fi, at_y, core].astype(jnp.float32)
                + landed[a, at_fi, at_y].astype(jnp.float32))

    for a in range(2):
        near(a).wait_recv()
        for k in range(len(others)):
            at_fi, at_y = spot(*others[k])
            pair_sum[a, at_fi, at_y] = joined(a, at_fi, at_y).astype(jnp.bfloat16)
            far(a, k).start()

    def owned(w, which):
        total = grads[w][fo, which].astype(jnp.float32)
        for step in range(1, n_fo):
            total += g_in[w, step - 1, which].astype(jnp.float32)
        return total

    for w in range(2):
        for step in range(1, n_fo):
            along(w, step).wait_recv()
        staged[w] = owned(w, 1 - fi).astype(jnp.bfloat16)
        across(w).start()
        mine[w][...] = owned(w, fi)
    for a in range(2):
        total = joined(a, fi, y)
        for k in range(len(others)):
            far(a, k).wait_recv()
            total += arrived[a, k].astype(jnp.float32)
        summed[a][...] = total.astype(jnp.bfloat16)
    for w in range(2):
        across(w).wait()
        for step in range(1, n_fo):
            along(w, step).wait_send()
    for a in range(2):
        near(a).wait_send()
        for k in range(len(others)):
            far(a, k).wait_send()


def reduce(n_fo, n_tp, partial, grads):
    rows, width = partial[0].shape[-2:]
    w_rows, half = grads[0].shape[-2:]
    n_y = n_tp // 2
    others = 2 * n_y - 1
    dma = pltpu.SemaphoreType.DMA
    bf16, f32 = jnp.bfloat16, jnp.float32
    return pl.pallas_call(
        functools.partial(reduce_kernel, n_fo, n_tp),
        out_shape=[jax.ShapeDtypeStruct((rows, width), bf16)] * 2
        + [jax.ShapeDtypeStruct((w_rows, half), f32)] * 2
        + [jax.ShapeDtypeStruct((w_rows, half), bf16)] * 2,
        in_specs=[VMEM] * 4,
        out_specs=[VMEM] * 6,
        scratch_shapes=[
            pltpu.VMEM((2, 2, n_y, rows, width), bf16),
            pltpu.VMEM((2, 2, n_y, rows, width), bf16),
            pltpu.VMEM((2, others, rows, width), bf16),
            pltpu.VMEM((2, n_fo - 1, 2, w_rows, half), bf16),
            pltpu.VMEM((2, w_rows, half), bf16),
            dma((2,)), dma((2,)), dma((2, others)), dma((2, others)),
            dma((2, n_fo - 1)), dma((2, n_fo - 1)), dma((2,)), dma((2,)),
        ],
        compiler_params=pltpu.CompilerParams(collective_id=1, has_side_effects=True),
        name="reduce",
    )(*partial, *grads)


def on_device(n_fo, n_tp, x_late, x_early, cotangent, up_weight, down_weight, up_grad_sum, down_grad_sum):
    rows, width = x_late.shape
    w_rows, cols = up_weight.shape
    half = cols // 2
    late, early, cot, up, down = gather(n_fo, n_tp, (x_late, x_early, cotangent), (up_weight, down_weight))
    late, early, cot = (a.reshape(-1, width) for a in (late, early, cot))
    up, down = (a.reshape(-1, half) for a in (up, down))
    pre_late = jnp.dot(late, up, preferred_element_type=jnp.float32)
    pre_early = jnp.dot(early, up, preferred_element_type=jnp.float32)
    act_late = squared(pre_late)
    grad_act = jnp.dot(cot, down, preferred_element_type=jnp.float32)
    act_early = squared(pre_early)
    grad_pre = hidden_grad(grad_act, pre_early)
    partial = [
        value.astype(jnp.bfloat16).reshape(2, n_tp // 2, 2, rows, width)
        for value in (dot_last(act_late, down), dot_last(grad_pre, up))
    ]
    grads = [
        value.astype(jnp.bfloat16).reshape(n_fo, 2, w_rows, half)
        for value in (dot_first(early, grad_pre), dot_first(cot, act_early))
    ]
    output, input_grad, up_mine, down_mine, up_other, down_other = reduce(n_fo, n_tp, partial, grads)
    low = lax.axis_index("fs") % 2 == 0

    def added(total, mine, other):
        other = other.astype(jnp.float32)
        return total + jnp.concatenate([jnp.where(low, mine, other), jnp.where(low, other, mine)], axis=1)

    return (output, input_grad, added(up_grad_sum, up_mine, up_other), added(down_grad_sum, down_mine, down_other))


def solution(mesh):
    rows, both = P(("fs", "tp"), None), P("fs", "tp")
    return jax.shard_map(
        functools.partial(on_device, mesh.shape["fs"] // 2, mesh.shape["tp"]),
        mesh=mesh,
        in_specs=(rows, rows, rows, both, both, both, both),
        out_specs=(rows, rows, both, both),
        check_vma=False,
    )
```

```python
import functools

import jax
import jax.numpy as jnp
from jax import lax
from jax.experimental import pallas as pl
from jax.experimental.pallas import tpu as pltpu
from jax.sharding import PartitionSpec as P


MESH = pl.DeviceIdType.MESH
ANY = pl.BlockSpec(memory_space=pl.ANY)
VMEM = pl.BlockSpec(memory_space=pltpu.VMEM)


def dot_last(left, right):
    return lax.dot_general(
        left, right, (((1,), (1,)), ((), ())), preferred_element_type=jnp.float32
    )


def dot_first(left, right):
    return lax.dot_general(
        left, right, (((0,), (0,)), ((), ())), preferred_element_type=jnp.float32
    )


def squared(pre_act):
    return jnp.square(jax.nn.relu(pre_act)).astype(jnp.bfloat16)


def hidden_grad(grad_act, pre_early):
    return (grad_act * 2.0 * jax.nn.relu(pre_early)).astype(jnp.bfloat16)


def flip(value, bit):
    return value + bit - 2 * bit * ((value // bit) % 2)


def remote(src, dst, send, recv, fs, tp):
    return pltpu.make_async_remote_copy(
        src_ref=src, dst_ref=dst, send_sem=send, recv_sem=recv,
        device_id={"fs": fs, "tp": tp}, device_id_type=MESH,
    )


def greet(peers):
    barrier = pltpu.get_barrier_semaphore()
    for fs, tp in peers:
        pl.semaphore_signal(barrier, inc=1, device_id={"fs": fs, "tp": tp}, device_id_type=MESH)
    pl.semaphore_wait(barrier, len(peers))


def gather_kernel(n_fo, n_tp, *refs):
    tokens, weights = refs[0:3], refs[3:5]
    all_tokens, all_weights = refs[5:8], refs[8:10]
    local, t_send, t_recv, x_send, x_recv, z_send, z_recv = refs[10:]
    fs, tp = lax.axis_index("fs"), lax.axis_index("tp")
    fo, fi = fs // 2, fs % 2
    pair = fo * 2 + 1 - fi
    half = weights[0].shape[1] // 2
    dims = n_tp.bit_length()

    def placed(mask):
        at_fi, at_tp = (1 - fi if mask & 1 else fi), tp
        for dim in range(1, dims):
            if (mask >> dim) & 1:
                at_tp = flip(at_tp, n_tp >> dim)
        return at_fi, at_tp

    def token(a, dim, mask):
        to_fi, to_tp = placed(1 << dim)
        slot = placed(mask)
        dst = all_tokens[a].at[slot[0], slot[1]]
        sem = mask + (1 << dim)
        return remote(tokens[a] if mask == 0 else dst, dst, t_send.at[a, sem], t_recv.at[a, sem],
                      fo * 2 + to_fi, to_tp)

    def columns(w, which):
        return weights[w].at[:, pl.ds(pl.multiple_of(which * half, half), half)]

    def across(w):
        return remote(columns(w, 1 - fi), all_weights[w].at[fs], x_send.at[w], x_recv.at[w], pair, tp)

    def along(w, source, part, way):
        dst = all_weights[w].at[source * 2 + (1 - fi if part else fi)]
        return dst, z_send.at[way, w, source, part], z_recv.at[w, source, part], ((fo + 1 - 2 * way) % n_fo) * 2 + fi

    def relay(w, source, part, way):
        dst, send, recv, to = along(w, source, part, way)
        return remote(dst, dst, send, recv, to, tp)

    def begin(w, way):
        dst, send, recv, to = along(w, fo, 0, way)
        return remote(columns(w, fi), dst, send, recv, to, tp)

    def open_way(way):
        return fo < n_fo - 1 if way == 0 else fo > 0

    def take(w, part, distance):
        for way in range(2):
            source = fo - distance if way == 0 else fo + distance

            @pl.when((source >= 0) & (source < n_fo))
            def _():
                relay(w, source, part, way).wait_recv()

                @pl.when(open_way(way))
                def _():
                    relay(w, source, part, way).start()

    peers = []
    for dim in range(dims):
        to_fi, to_tp = placed(1 << dim)
        peers.append((fo * 2 + to_fi, to_tp))
    for step in (1, n_fo - 1):
        peers.append((((fo + step) % n_fo) * 2 + fi, tp))
    greet(peers)

    for way in range(2):
        @pl.when(open_way(way))
        def _():
            for w in range(2):
                begin(w, way).start()
    for a in range(3):
        token(a, 0, 0).start()
        if a < 2:
            across(a).start()
    for a in range(3):
        for dim in range(1, dims):
            token(a, dim, 0).start()
    own = [pltpu.make_async_copy(tokens[a], all_tokens[a].at[fi, tp], local.at[a]) for a in range(3)]
    own += [pltpu.make_async_copy(columns(w, fi), all_weights[w].at[fs], local.at[3 + w]) for w in range(2)]
    for copy in own:
        copy.start()

    def passed(a, dim, mask):
        token(a, dim, mask).wait_recv()
        for later in range(dim + 1, dims):
            token(a, later, mask + (1 << dim)).start()

    def crossed(w):
        across(w).wait_recv()
        for way in range(2):
            @pl.when(open_way(way))
            def _():
                relay(w, fo, 1, way).start()

    take(0, 0, 1)
    take(1, 0, 1)
    passed(0, 0, 0)
    crossed(0)
    for distance in range(2, n_fo):
        take(0, 0, distance)
        take(1, 0, distance)
        if distance == 2:
            passed(1, 0, 0)
            crossed(1)
            take(0, 1, 1)
            passed(2, 0, 0)
    take(1, 1, 1)
    for distance in range(2, n_fo - 1):
        take(0, 1, distance)
        take(1, 1, distance)
    for dim in range(1, dims):
        for mask in range(1 << dim):
            for a in range(3):
                passed(a, dim, mask)
    for w in range(2):
        take(w, 1, n_fo - 1)
        across(w).wait_send()
        for way in range(2):
            @pl.when(open_way(way))
            def _():
                begin(w, way).wait_send()
                relay(w, fo, 1, way).wait_send()
                for distance in range(1, n_fo):
                    source = fo - distance if way == 0 else fo + distance

                    @pl.when((source >= 0) & (source < n_fo))
                    def _():
                        for part in range(2):
                            relay(w, source, part, way).wait_send()
    for dim in range(dims):
        for a in range(3):
            for mask in range(1 << dim):
                token(a, dim, mask).wait_send()
    for copy in own:
        copy.wait()


def gather(n_fo, n_tp, tokens, weights):
    rows, width = tokens[0].shape
    w_rows, cols = weights[0].shape
    masks = 2 * n_tp
    dma = pltpu.SemaphoreType.DMA
    return pl.pallas_call(
        functools.partial(gather_kernel, n_fo, n_tp),
        out_shape=[jax.ShapeDtypeStruct((2, n_tp, rows, width), jnp.bfloat16)] * 3
        + [jax.ShapeDtypeStruct((2 * n_fo, w_rows, cols // 2), jnp.bfloat16)] * 2,
        in_specs=[VMEM] * 5,
        out_specs=[ANY] * 5,
        scratch_shapes=[
            dma((5,)), dma((3, masks)), dma((3, masks)), dma((2,)), dma((2,)),
            dma((2, 2, n_fo, 2)), dma((2, n_fo, 2)),
        ],
        compiler_params=pltpu.CompilerParams(collective_id=0, has_side_effects=True),
        name="gather",
    )(*tokens, *weights)


def reduce_kernel(n_fo, n_tp, *refs):
    partial, grads = refs[0:2], refs[2:4]
    summed, mine, other = refs[4:6], refs[6:8], refs[8:10]
    (landed, pair_sum, arrived, g_in, staged,
     c_send, c_recv, t_send, t_recv, z_send, z_recv, x_send, x_recv) = refs[10:]
    fs, tp = lax.axis_index("fs"), lax.axis_index("tp")
    fo, fi = fs // 2, fs % 2
    pair = fo * 2 + 1 - fi
    n_y = n_tp // 2
    y, core = tp // 2, tp % 2
    others = [(dx, dy) for dy in range(n_y) for dx in range(2) if (dx, dy) != (0, 0)]

    def spot(dx, dy):
        return (1 - fi if dx else fi), (y + dy) % n_y

    def near(a):
        return remote(partial[a].at[:, :, 1 - core], landed.at[a], c_send.at[a], c_recv.at[a],
                      fs, y * 2 + 1 - core)

    def far(a, k):
        at_fi, at_y = spot(*others[k])
        return remote(pair_sum.at[a, at_fi, at_y], arrived.at[a, k], t_send.at[a, k], t_recv.at[a, k],
                      fo * 2 + at_fi, at_y * 2 + core)

    def along(w, block, way, src):
        return remote(src, g_in.at[way, w, block], z_send.at[way, w, block], z_recv.at[way, w, block],
                      ((fo + 1 - 2 * way) % n_fo) * 2 + fi, tp)

    def onward(way, distance, action):
        block = fo + distance if way == 0 else fo - distance
        first = fo == 0 if way == 0 else fo == n_fo - 1
        inside = (block >= 0) & (block < n_fo)
        for w in range(2):
            action(w, block, first, inside)

    def across(w):
        return remote(staged.at[w], other[w], x_send.at[w], x_recv.at[w], pair, tp)

    peers = [(fs, y * 2 + 1 - core)]
    for dx, dy in others:
        at_fi, at_y = spot(dx, dy)
        peers.append((fo * 2 + at_fi, at_y * 2 + core))
    for step in (1, n_fo - 1):
        peers.append((((fo + step) % n_fo) * 2 + fi, tp))
    greet(peers)

    for a in range(2):
        near(a).start()
    for way in range(2):
        def launch(w, block, first, inside):
            @pl.when(first & inside)
            def _():
                along(w, block, way, grads[w].at[block]).start()

        for distance in range(n_fo - 1, 0, -1):
            onward(way, distance, launch)

    def joined(a, at_fi, at_y):
        return (partial[a][at_fi, at_y, core].astype(jnp.float32)
                + landed[a, at_fi, at_y].astype(jnp.float32))

    for a in range(2):
        near(a).wait_recv()
        for k in range(len(others)):
            at_fi, at_y = spot(*others[k])
            pair_sum[a, at_fi, at_y] = joined(a, at_fi, at_y).astype(jnp.bfloat16)
            far(a, k).start()

    for distance in range(n_fo - 2, 0, -1):
        for way in range(2):
            def carry(w, block, first, inside):
                @pl.when(jnp.logical_not(first) & inside)
                def _():
                    held = g_in.at[way, w, block]
                    along(w, block, way, held).wait_recv()
                    for part in range(2):
                        g_in[way, w, block, part] = (
                            grads[w][block, part].astype(jnp.float32)
                            + g_in[way, w, block, part].astype(jnp.float32)
                        ).astype(jnp.bfloat16)
                    along(w, block, way, held).start()

            onward(way, distance, carry)

    def owned(w, which):
        return (grads[w][fo, which].astype(jnp.float32)
                + g_in[0, w, fo, which].astype(jnp.float32)
                + g_in[1, w, fo, which].astype(jnp.float32))

    for w in range(2):
        for way in range(2):
            first = fo == 0 if way == 0 else fo == n_fo - 1

            @pl.when(first)
            def _():
                g_in[way, w, fo] = jnp.zeros(g_in.shape[3:], g_in.dtype)

            @pl.when(jnp.logical_not(first))
            def _():
                along(w, fo, way, g_in.at[way, w, fo]).wait_recv()
        staged[w] = owned(w, 1 - fi).astype(jnp.bfloat16)
        across(w).start()
        mine[w][...] = owned(w, fi)
    for a in range(2):
        total = joined(a, fi, y)
        for k in range(len(others)):
            far(a, k).wait_recv()
            total += arrived[a, k].astype(jnp.float32)
        summed[a][...] = total.astype(jnp.bfloat16)
    for w in range(2):
        across(w).wait()
    for way in range(2):
        def finish(w, block, first, inside):
            @pl.when(inside)
            def _():
                along(w, block, way, grads[w].at[block]).wait_send()

        for distance in range(n_fo - 1, 0, -1):
            onward(way, distance, finish)
    for a in range(2):
        near(a).wait_send()
        for k in range(len(others)):
            far(a, k).wait_send()


def reduce(n_fo, n_tp, partial, grads):
    rows, width = partial[0].shape[-2:]
    w_rows, half = grads[0].shape[-2:]
    n_y = n_tp // 2
    others = 2 * n_y - 1
    dma = pltpu.SemaphoreType.DMA
    bf16, f32 = jnp.bfloat16, jnp.float32
    return pl.pallas_call(
        functools.partial(reduce_kernel, n_fo, n_tp),
        out_shape=[jax.ShapeDtypeStruct((rows, width), bf16)] * 2
        + [jax.ShapeDtypeStruct((w_rows, half), f32)] * 2
        + [jax.ShapeDtypeStruct((w_rows, half), bf16)] * 2,
        in_specs=[VMEM] * 4,
        out_specs=[VMEM] * 6,
        scratch_shapes=[
            pltpu.VMEM((2, 2, n_y, rows, width), bf16),
            pltpu.VMEM((2, 2, n_y, rows, width), bf16),
            pltpu.VMEM((2, others, rows, width), bf16),
            pltpu.VMEM((2, 2, n_fo, 2, w_rows, half), bf16),
            pltpu.VMEM((2, w_rows, half), bf16),
            dma((2,)), dma((2,)), dma((2, others)), dma((2, others)),
            dma((2, 2, n_fo)), dma((2, 2, n_fo)), dma((2,)), dma((2,)),
        ],
        compiler_params=pltpu.CompilerParams(collective_id=1, has_side_effects=True),
        name="reduce",
    )(*partial, *grads)


def on_device(n_fo, n_tp, x_late, x_early, cotangent, up_weight, down_weight, up_grad_sum, down_grad_sum):
    rows, width = x_late.shape
    w_rows, cols = up_weight.shape
    half = cols // 2
    late, early, cot, up, down = gather(n_fo, n_tp, (x_late, x_early, cotangent), (up_weight, down_weight))
    late, early, cot = (a.reshape(-1, width) for a in (late, early, cot))
    up, down = (a.reshape(-1, half) for a in (up, down))
    pre_late = jnp.dot(late, up, preferred_element_type=jnp.float32)
    pre_early = jnp.dot(early, up, preferred_element_type=jnp.float32)
    act_late = squared(pre_late)
    grad_act = jnp.dot(cot, down, preferred_element_type=jnp.float32)
    act_early = squared(pre_early)
    grad_pre = hidden_grad(grad_act, pre_early)
    partial = [
        value.astype(jnp.bfloat16).reshape(2, n_tp // 2, 2, rows, width)
        for value in (dot_last(act_late, down), dot_last(grad_pre, up))
    ]
    grads = [
        value.astype(jnp.bfloat16).reshape(n_fo, 2, w_rows, half)
        for value in (dot_first(early, grad_pre), dot_first(cot, act_early))
    ]
    output, input_grad, up_mine, down_mine, up_other, down_other = reduce(n_fo, n_tp, partial, grads)
    low = lax.axis_index("fs") % 2 == 0

    def added(total, mine, other):
        other = other.astype(jnp.float32)
        return total + jnp.concatenate([jnp.where(low, mine, other), jnp.where(low, other, mine)], axis=1)

    return (output, input_grad, added(up_grad_sum, up_mine, up_other), added(down_grad_sum, down_mine, down_other))


def solution(mesh):
    rows, both = P(("fs", "tp"), None), P("fs", "tp")
    return jax.shard_map(
        functools.partial(on_device, mesh.shape["fs"] // 2, mesh.shape["tp"]),
        mesh=mesh,
        in_specs=(rows, rows, rows, both, both, both, both),
        out_specs=(rows, rows, both, both),
        check_vma=False,
    )
```
